32 devices in a mesh: sp: 16 (over z, y, x), tp: 2 (over core).
Axes of the slice: x: 2, y: 2, z: 4, core: 2. Of those that a mesh axis runs over, the one named last changes fastest.
Arguments:
- residual: bfloat16 [2048, 2048], P('sp'), may hold values from -6 to 6
- query_proj: bfloat16 [2048, 1024], P('sp', 'tp'), may hold values from -6 to 6
- key_proj: bfloat16 [2048, 1024], P('sp', 'tp'), may hold values from -6 to 6
- value_proj: bfloat16 [2048, 2048], P('sp', 'tp'), may hold values from -6 to 6
- out_gate: bfloat16 [2048, 2048], P('sp', 'tp'), may hold values from -6 to 6
- log_decay: float32 [2048, 1024], P('sp', 'tp'), may hold values from -1 to 0
- doc_ids: int32 [2048], P('sp'), may hold values from 0 to 3, never falling along the last dimension, each value on 1 to 1536 neighbouring positions
- head_gain: float32 [8, 256], P('tp'), may hold values from 0.1 to 1.9
- w_out: bfloat16 [2048, 2048], P('tp'), may hold values from -0.125 to 0.125
- ffn_gain: float32 [2048], replicated, may hold values from 0.1 to 1.9
- w_gate: bfloat16 [2048, 5120], P('sp', 'tp'), may hold values from -0.125 to 0.125
- w_value: bfloat16 [2048, 5120], P('sp', 'tp'), may hold values from -0.125 to 0.125
- w_down_t: bfloat16 [2048, 5120], P('sp', 'tp'), may hold values from -0.078125 to 0.078125
- conv_taps: float32 [3, 2, 5120], P(None, None, 'tp'), may hold values from -3.5 to 3.5
- conv_bias: float32 [2, 5120], P(None, 'tp'), may hold values from -3 to 3
Outputs:
- result: bfloat16 [2048, 2048], P('sp')
The draws below stay inside these ranges and needn't reach their ends.
Inputs may be any that keep to these rules, and one draw needn't show every extreme that they name: `doc_ids`: document numbers never fall along the sequence; each document holds 1 to 1536 positions, and one holds exactly 1536.
All inputs are finite; a program needn't handle non-finite values.
Results may differ from the reference program's by a relative error of at most 0.017.
Values may be sent and summed in bfloat16 or wider, within the bound.
A program may use at most 128 MiB of HBM per device.

```python
import math
import jax
import jax.numpy as jnp
import numpy as np
from jax import lax

D = 2048
H = 8
DK = 128
DV = 256
FF = 5120
BLOCK = 64
SPAN_LENGTH = 2048
GROUPS = 2
DOCS = 4
DOC_MOST = 1536


def draw_log_decay(key, part):
    packed_texts_batch = jax.random.split(key, 6)
    feature_dimension = H * DK
    slow_share = 0.5
    slow_heads = jax.random.uniform(packed_texts_batch[0], (H,), jnp.float32) < slow_share
    slow_chan = jnp.repeat(slow_heads, DK)
    channel = jnp.exp(jax.random.uniform(packed_texts_batch[1], (feature_dimension,), jnp.float32, -0.7, 0.7))
    fading_speed_reference = jnp.where(slow_chan, 0.7 / SPAN_LENGTH, 1.0 / 40.0) * channel
    segment_fade_multiplier = jnp.exp(jax.random.uniform(packed_texts_batch[2], (SPAN_LENGTH // BLOCK, 1), jnp.float32, -0.7, 0.7))
    segment_fade_multiplier = jnp.repeat(segment_fade_multiplier, BLOCK, axis=0)
    approximate_guess = jax.random.uniform(packed_texts_batch[3], (SPAN_LENGTH, feature_dimension), jnp.float32, 0.5, 1.5)
    spots = jax.random.randint(packed_texts_batch[4], (3,), 0, SPAN_LENGTH)
    removed_elements = jnp.any(jnp.arange(SPAN_LENGTH)[:, None] == spots[None, :], axis=1)
    word_piece_group = jnp.log(jax.random.uniform(packed_texts_batch[5], (SPAN_LENGTH, feature_dimension), jnp.float32, 0.6, 0.85))
    return -fading_speed_reference * segment_fade_multiplier * approximate_guess + jnp.where(removed_elements[:, None], word_piece_group, 0.0)


def block_scale(stream_key, extent, cuts, low, high):
    def one(axis_at, shards_of):
        draws = jax.random.uniform(jax.random.fold_in(jax.random.fold_in(stream_key, 6), axis_at), (shards_of,), jnp.float32, low / len(cuts), high / len(cuts))
        return jnp.repeat(jnp.exp(draws), extent[axis_at] // shards_of).reshape((-1,) + (1,) * (len(extent) - axis_at - 1))

    loudness = one(*cuts[0])
    for cut in cuts[1:]:
        loudness = loudness * one(*cut)
    return loudness


def profile(number_of, total, reach, slope):
    portions = [(1 << 20) // math.isqrt(standing ** slope) + 1 for standing in range(2, number_of + 1)]
    rest, holding = total - reach - (number_of - 1), [1] * (number_of - 1)
    while rest > 0:
        movable = [i for i in range(number_of - 1) if holding[i] < reach]
        mass, left = sum([portions[i] for i in movable]), rest
        for i in movable:
            extra = min(reach - holding[i], max(1, left * portions[i] // mass), rest)
            holding[i] = holding[i] + extra
            rest = rest - extra
    return np.array([reach] + holding)


def uneven(rng, amount, total, bound, slope):
    if amount == 2:
        one = jax.random.randint(rng, (), max(1, total - bound), min(bound, total - 1) + 1)
        return jnp.stack([one, total - one])
    lengths = jnp.asarray(profile(amount, total, bound, slope), jnp.int32)
    pairs = (amount - 1) // 2
    source_of, taker = lengths[1:1 + 2 * pairs:2], lengths[2:2 + 2 * pairs:2]
    slack = jnp.minimum(source_of - 1, bound - taker)
    passed = jax.random.randint(jax.random.fold_in(rng, 1), (pairs,), 0, 1 << 20) % (slack + 1)
    lengths = lengths.at[1:1 + 2 * pairs:2].set(source_of - passed).at[2:2 + 2 * pairs:2].set(taker + passed)
    return lengths[jax.random.permutation(jax.random.fold_in(rng, 2), amount)]


def centred(rng, shape, scale, most, cuts=(), held_as=jnp.bfloat16):
    values = jax.random.normal(rng, shape, jnp.float32) * scale
    if len(cuts) > 0:
        values = block_scale(rng, shape, cuts, -0.22, 0.18) * values
    return jnp.clip(values, min=-most, max=most).astype(held_as)


def setup_inputs(seed: int = 0) -> dict:
    arg_keys = jax.random.split(jax.random.key(seed), 16)
    residual = centred(arg_keys[0], (SPAN_LENGTH, D), 1.0, 6.0, ((0, 16),))
    query_proj = centred(arg_keys[1], (SPAN_LENGTH, H * DK), 1.0, 6.0, ((0, 16), (1, 2)))
    key_proj = centred(arg_keys[2], (SPAN_LENGTH, H * DK), 1.0, 6.0, ((0, 16), (1, 2)))
    value_proj = centred(arg_keys[3], (SPAN_LENGTH, H * DV), 1.0, 6.0, ((0, 16), (1, 2)))
    out_gate = centred(arg_keys[4], (SPAN_LENGTH, H * DV), 1.0, 6.0, ((0, 16), (1, 2)))
    log_decay = draw_log_decay(jax.random.fold_in(arg_keys[15], 71), 0)
    doc_ids = jnp.searchsorted(jnp.cumsum(uneven(arg_keys[6], DOCS, SPAN_LENGTH, DOC_MOST, 0)), jnp.arange(SPAN_LENGTH), side="right").astype(jnp.int32)
    head_gain = jnp.clip(1.0 + 0.18 * jax.random.normal(arg_keys[7], (H, DV), jnp.float32), 0.1, 1.9)
    w_out = centred(arg_keys[8], (H * DV, D), (H * DV) ** -0.5, 0.125, ((0, 2),))
    ffn_gain = jnp.clip(1.0 + 0.18 * jax.random.normal(arg_keys[9], (D,), jnp.float32), 0.1, 1.9)
    w_gate = centred(arg_keys[10], (D, FF), D ** -0.5, 0.125, ((0, 16), (1, 2)))
    w_value = centred(arg_keys[11], (D, FF), D ** -0.5, 0.125, ((0, 16), (1, 2)))
    w_down_t = centred(arg_keys[12], (D, FF), FF ** -0.5, 0.078125, ((0, 16), (1, 2)))
    conv_taps = centred(arg_keys[13], (3, 2, FF), 3 ** -0.5, 3.5, ((2, 2),), jnp.float32)
    conv_bias = centred(arg_keys[14], (2, FF), 0.5, 3.0, ((1, 2),), jnp.float32)
    return {"residual": residual, "query_proj": query_proj, "key_proj": key_proj, "value_proj": value_proj, "out_gate": out_gate, "log_decay": log_decay, "doc_ids": doc_ids, "head_gain": head_gain, "w_out": w_out, "ffn_gain": ffn_gain, "w_gate": w_gate, "w_value": w_value, "w_down_t": w_down_t, "conv_taps": conv_taps, "conv_bias": conv_bias}


EPS = 1e-06

def mix_positions(projected, doc_ids, conv_taps, conv_bias, branch_idx):
    values = projected.astype(jnp.float32)
    lag_one = jnp.pad(values, ((1, 0), (0, 0)))[:-1]
    lag_two = jnp.pad(values, ((2, 0), (0, 0)))[:-2]
    doc_one = jnp.pad(doc_ids, (1, 0), constant_values=-1)[:-1]
    doc_two = jnp.pad(doc_ids, (2, 0), constant_values=-1)[:-2]
    mask_one = (doc_one == doc_ids).astype(jnp.float32)[:, None]
    mask_two = (doc_two == doc_ids).astype(jnp.float32)[:, None]
    return conv_bias[branch_idx] + conv_taps[2, branch_idx] * values + conv_taps[1, branch_idx] * lag_one * mask_one + conv_taps[0, branch_idx] * lag_two * mask_two

def reference(residual, query_proj, key_proj, value_proj, out_gate, log_decay, doc_ids, head_gain, w_out, ffn_gain, w_gate, w_value, w_down_t, conv_taps, conv_bias):
    highest_precision = lax.Precision.HIGHEST
    number = SPAN_LENGTH // BLOCK

    def blocks(source, feature_dimension):
        return source.astype(jnp.float32).reshape(number, BLOCK, H, feature_dimension).transpose(0, 2, 1, 3)
    q_blocks = blocks(query_proj, DK) * DK ** (-0.5)
    k_blocks = blocks(key_proj, DK)
    v_blocks = blocks(value_proj, DV)
    g_blocks = blocks(log_decay, DK)
    d_blocks = doc_ids.reshape(number, BLOCK)
    causal = jnp.tril(jnp.ones((BLOCK, BLOCK), bool))

    def advance(carried_in, inputs):
        state_sequence, before = carried_in
        current_queries, current_keys, current_values, g_now, d_now = inputs
        cumulative_log_decay = jnp.cumsum(g_now, axis=1)
        keep_mask = (d_now == before).astype(jnp.float32)
        carried_state = jnp.einsum('obl,olx->obx', current_queries * jnp.exp(cumulative_log_decay), state_sequence, precision=highest_precision)
        carried_state = carried_state * keep_mask[None, :, None]
        same_doc = causal & (d_now[:, None] == d_now[None, :])
        log_gap = cumulative_log_decay[:, :, None, :] - cumulative_log_decay[:, None, :, :]
        weight = jnp.where(same_doc[None, :, :, None], jnp.exp(jnp.minimum(log_gap, 0.0)), 0.0)
        scores = jnp.einsum('htk,hsk,htsk->hts', current_queries, current_keys, weight, precision=highest_precision)
        within = jnp.einsum('hts,hsv->htv', scores, current_values, precision=highest_precision)
        total_log_decay = cumulative_log_decay[:, -1, :]
        trailing_mask = (d_now == d_now[-1]).astype(jnp.float32)
        initial_state = jnp.einsum('cxu,cxg->cug', current_keys * jnp.exp(total_log_decay[:, None, :] - cumulative_log_decay) * trailing_mask[None, :, None], current_values, precision=highest_precision)
        state_sequence = state_sequence * (jnp.exp(total_log_decay) * keep_mask[-1])[:, :, None] + initial_state
        return ((state_sequence, d_now[-1]), carried_state + within)
    start = (jnp.zeros((H, DK, DV), jnp.float32), jnp.array(-1, jnp.int32))
    _, block_out = lax.scan(advance, start, (q_blocks, k_blocks, v_blocks, g_blocks, d_blocks))
    head_out = block_out.transpose(0, 2, 1, 3).reshape(SPAN_LENGTH, H, DV)
    head_out = head_out * lax.rsqrt(lax.optimization_barrier(jnp.mean(head_out * head_out, axis=-1, keepdims=True)) + EPS) * head_gain
    mixed_heads = (head_out.reshape(SPAN_LENGTH, H * DV) * jax.nn.silu(out_gate.astype(jnp.float32))).astype(jnp.bfloat16)
    group_cols = H * DV // GROUPS
    attn_sum = jnp.zeros((SPAN_LENGTH, D), jnp.float32)
    for member in range(GROUPS):
        term = jnp.dot(mixed_heads[:, member * group_cols:(member + 1) * group_cols], w_out[member * group_cols:(member + 1) * group_cols], preferred_element_type=jnp.float32)
        attn_sum = attn_sum + term.astype(jnp.bfloat16).astype(jnp.float32)
    stream = (residual.astype(jnp.float32) + attn_sum).astype(jnp.bfloat16)
    stream_f = stream.astype(jnp.float32)
    normed = (stream_f * lax.rsqrt(lax.optimization_barrier(jnp.mean(stream_f * stream_f, axis=-1, keepdims=True)) + EPS) * ffn_gain).astype(jnp.bfloat16)
    gate_up = jnp.dot(normed, w_gate, preferred_element_type=jnp.float32).astype(jnp.bfloat16)
    value_up = jnp.dot(normed, w_value, preferred_element_type=jnp.float32).astype(jnp.bfloat16)
    gate_mix = mix_positions(gate_up, doc_ids, conv_taps, conv_bias, 0)
    value_mix = mix_positions(value_up, doc_ids, conv_taps, conv_bias, 1)
    hidden = (jax.nn.silu(gate_mix) * value_mix).astype(jnp.bfloat16)
    group_units = FF // GROUPS
    ffn_sum = jnp.zeros((SPAN_LENGTH, D), jnp.float32)
    for member in range(GROUPS):
        cols = slice(member * group_units, (member + 1) * group_units)
        term = lax.dot_general(hidden[:, cols], w_down_t[:, cols], (((1,), (1,)), ((), ())), preferred_element_type=jnp.float32)
        ffn_sum = ffn_sum + term.astype(jnp.bfloat16).astype(jnp.float32)
    return (stream_f + ffn_sum).astype(jnp.bfloat16)
```

```python
import functools

import jax
import jax.numpy as jnp
from jax import lax
from jax.experimental import pallas as pl
from jax.experimental.pallas import tpu as pltpu
from jax.sharding import PartitionSpec as P

EPS = 1e-06
VMEM = pl.BlockSpec(memory_space=pltpu.VMEM)
HIGH = lax.Precision.HIGHEST
BF = jnp.bfloat16
F32 = jnp.float32


def plane_count(positions, hidden):
    return max(b for b in (1, 2, 4) if positions % b == 0 and (hidden // b) % 128 == 0)


def nt(a, b):
    return lax.dot_general(a, b, (((1,), (1,)), ((), ())), preferred_element_type=F32)


def tn(a, b):
    return lax.dot_general(a, b, (((0,), (0,)), ((), ())), preferred_element_type=F32)


def local_kernel(heads, q_ref, k_ref, v_ref, g_ref, dcol_ref, drow_ref, o_ref, s_ref, qd_ref, cum_ref):
    rows = q_ref.shape[0]
    dk = q_ref.shape[1] // heads
    dv = v_ref.shape[1] // heads
    half = rows // 2
    t = lax.broadcasted_iota(jnp.int32, (rows, rows), 0)
    s = lax.broadcasted_iota(jnp.int32, (rows, rows), 1)
    tril = (t >= s).astype(F32)
    cum_ref[...] = jnp.dot(tril, g_ref[...], precision=HIGH, preferred_element_type=F32)
    dcol = dcol_ref[...]
    allowed = (t >= s) & (dcol == drow_ref[...])
    tail = (dcol == dcol_ref[rows - 1:rows, :]).astype(F32)
    scale = dk ** -0.5
    for h in range(heads):
        kc = pl.ds(h * dk, dk)
        vc = pl.ds(h * dv, dv)
        cum = cum_ref[:, kc]
        q = q_ref[:, kc].astype(F32) * scale
        k = k_ref[:, kc].astype(F32)
        v = v_ref[:, vc]
        total = cum[rows - 1:rows, :]
        qd_ref[:, kc] = (q * jnp.exp(cum)).astype(BF)
        s_ref[kc, :] = tn((k * jnp.exp(total - cum) * tail).astype(BF), v).astype(BF)
        edge = cum[half - 1:half, :]
        for part in range(2):
            rs = slice(part * half, (part + 1) * half)
            mid = cum[part * half + half // 2 - 1:part * half + half // 2, :]
            qs = (q[rs] * jnp.exp(cum[rs] - mid)).astype(BF)
            ks = (k[rs] * jnp.exp(mid - cum[rs])).astype(BF)
            a = jnp.where(allowed[rs, rs], nt(qs, ks), 0.0).astype(BF)
            o = jnp.dot(a, v[rs], preferred_element_type=F32)
            if part == 1:
                qx = (q[rs] * jnp.exp(cum[rs] - edge)).astype(BF)
                kx = (k[:half] * jnp.exp(edge - cum[:half])).astype(BF)
                x = jnp.where(allowed[rs, :half], nt(qx, kx), 0.0).astype(BF)
                o = o + jnp.dot(x, v[:half], preferred_element_type=F32)
            o_ref[rs, vc] = o


def out_kernel(heads, o_ref, qd_ref, p_ref, reach_ref, gate_ref, gain_ref, w_ref, out_ref, mixed):
    dk = qd_ref.shape[1] // heads
    dv = o_ref.shape[1] // heads
    for h in range(heads):
        kc = pl.ds(h * dk, dk)
        vc = pl.ds(h * dv, dv)
        carried = jnp.dot(qd_ref[:, kc], p_ref[kc, :], preferred_element_type=F32)
        head = o_ref[:, vc] + carried * reach_ref[...]
        head = head * lax.rsqrt(jnp.mean(head * head, axis=-1, keepdims=True) + EPS) * gain_ref[h:h + 1, :]
        gate = gate_ref[:, vc].astype(F32)
        mixed[:, vc] = (head * gate / (1.0 + jnp.exp(-gate))).astype(BF)
    out_ref[...] = jnp.dot(mixed[...], w_ref[...], preferred_element_type=F32).astype(BF)


def rotate(value, count, stride_in, size, steps):
    perm = []
    for i in range(count):
        d = (i // stride_in) % size
        perm.append((i, i + (((d + steps) % size) - d) * stride_in))
    return lax.ppermute(value, "sp", perm)


def swap(value):
    n = lax.axis_size("tp")
    return [lax.ppermute(value, "tp", [(i, (i + k) % n) for i in range(n)]) for k in range(1, n)]


def tp_gather(value):
    n = lax.axis_size("tp")
    if n != 2:
        return lax.all_gather(value, "tp", axis=0)
    (other,) = swap(value)
    first = lax.axis_index("tp") == 0
    return jnp.stack([jnp.where(first, value, other), jnp.where(first, other, value)])


def tp_scatter(value):
    n = lax.axis_size("tp")
    if n != 2:
        return lax.psum_scatter(value, "tp", scatter_dimension=0, tiled=False).astype(F32)
    c = lax.axis_index("tp")
    give = lax.dynamic_index_in_dim(value, 1 - c, 0, False)
    keep = lax.dynamic_index_in_dim(value, c, 0, False)
    return keep.astype(F32) + swap(give)[0].astype(F32)


def ordered(own, received, place, size):
    buf = jnp.zeros((size,) + own.shape, own.dtype)
    buf = lax.dynamic_update_index_in_dim(buf, own, place, 0)
    for k, item in enumerate(received, 1):
        buf = lax.dynamic_update_index_in_dim(buf, item, (place - k) % size, 0)
    return buf


def plane_gather(block, count, m, r, groups):
    if m != 4:
        return lax.all_gather(block, "sp", axis=0, tiled=True, axis_index_groups=groups)
    half = block.shape[0] // 2
    near = rotate(block, count, 1, 2, 1)
    far = rotate(block, count, 2, 2, 1)
    diag_top = rotate(near[:half], count, 2, 2, 1)
    diag_low = rotate(far[half:], count, 1, 2, 1)
    x, y = r % 2, r // 2
    at = lambda i, j: (2 * j + i) * 2 * half
    buf = jnp.zeros((m * 2 * half, block.shape[1]), block.dtype)
    buf = lax.dynamic_update_slice_in_dim(buf, block, at(x, y), 0)
    buf = lax.dynamic_update_slice_in_dim(buf, near, at(1 - x, y), 0)
    buf = lax.dynamic_update_slice_in_dim(buf, far, at(x, 1 - y), 0)
    buf = lax.dynamic_update_slice_in_dim(buf, diag_top, at(1 - x, 1 - y), 0)
    return lax.dynamic_update_slice_in_dim(buf, diag_low, at(1 - x, 1 - y) + half, 0)


def per_device(residual, query_proj, key_proj, value_proj, out_gate, log_decay, doc_ids, head_gain,
               w_out, ffn_gain, w_gate, w_value, w_down_t, conv_taps, conv_bias):
    count = lax.axis_size("sp")
    rows = doc_ids.shape[0]
    heads = head_gain.shape[0]
    dk = query_proj.shape[1] // heads
    dv = value_proj.shape[1] // heads
    depth, hidden_here = w_gate.shape
    width = residual.shape[1]
    b = plane_count(count, hidden_here)
    m = count // b
    fc = hidden_here // b
    place = lax.axis_index("sp")
    z, r = place // m, place % m
    groups = [[g * m + i for i in range(m)] for g in range(b)]

    note = jnp.concatenate([jnp.sum(log_decay, axis=0), doc_ids.astype(F32)])
    notes = lax.all_gather(note, "sp", axis=0)
    w_gate, w_value, notes = lax.optimization_barrier((w_gate, w_value, notes))

    def chunk(w, j):
        return lax.dynamic_slice_in_dim(w, j * fc, fc, 1)

    def exchange(pick):
        received = [rotate(pick((z + k) % b), count, m, b, k) for k in range(1, b)]
        block = ordered(pick(z), received, z, b).reshape(b * depth, -1)
        return plane_gather(block, count, m, r, groups)

    up_w = exchange(lambda j: jnp.concatenate([chunk(w_gate, j), chunk(w_value, j)], axis=1))

    totals, docs = notes[:, :heads * dk], notes[:, heads * dk:]
    first, last = docs[:, 0], docs[:, -1]
    steps = jnp.arange(count)

    o_local, state, q_dec = pl.pallas_call(
        functools.partial(local_kernel, heads),
        out_shape=(
            jax.ShapeDtypeStruct((rows, heads * dv), F32),
            jax.ShapeDtypeStruct((heads * dk, dv), BF),
            jax.ShapeDtypeStruct((rows, heads * dk), BF),
        ),
        in_specs=[VMEM] * 6,
        out_specs=(VMEM,) * 3,
        scratch_shapes=[pltpu.VMEM((rows, heads * dk), F32)],
        cost_estimate=pl.CostEstimate(flops=10**9, bytes_accessed=3 * 10**6, transcendentals=0),
    )(query_proj, key_proj, value_proj, log_decay, doc_ids[:, None], doc_ids[None, :])

    def weight(source, until):
        inside = (steps > source) & (steps < until)
        return jnp.exp(jnp.sum(jnp.where(inside[:, None], totals, 0.0), axis=0))

    my_first = first[place]
    if b == 1:
        all_states = lax.all_gather(state, "sp", axis=0)

        def add(i, acc):
            live = (i < place) & (last[i] == my_first)
            scale = jnp.where(live, weight(i, place), 0.0)
            return acc + scale[:, None] * all_states[i].astype(F32)

        prefix = lax.fori_loop(0, count, add, jnp.zeros(state.shape, F32))
    else:
        near = [state] + [rotate(state, count, 1, m, k) for k in range(1, m)]
        prefix = jnp.zeros(state.shape, F32)
        plane_end = jnp.zeros(state.shape, F32)
        end = (z + 1) * m
        end_doc = last[end - 1]
        for k, item in enumerate(near):
            source_r = (r - k) % m
            source = z * m + source_r
            if k:
                live = (source_r < r) & (last[source] == my_first)
                prefix += jnp.where(live, weight(source, place), 0.0)[:, None] * item.astype(F32)
            scale = jnp.where(last[source] == end_doc, weight(source, end), 0.0)
            plane_end += scale[:, None] * item.astype(F32)
        plane_end = plane_end.astype(BF)
        whole = jnp.zeros(state.shape, F32)
        for k in range(1, b):
            item = lax.ppermute(plane_end, "sp", [(i, i + k * m) for i in range(count - k * m)])
            source_end = jnp.maximum(z - k + 1, 0) * m - 1
            live = (z >= k) & (last[source_end] == first[z * m])
            scale = jnp.where(live, weight(source_end, z * m), 0.0)
            whole += scale[:, None] * item.astype(F32)
        reach = jnp.where(first[z * m] == my_first, weight(z * m - 1, place), 0.0)
        prefix += reach[:, None] * whole

    prefix = prefix.astype(BF)
    w_down_t, prefix = lax.optimization_barrier((w_down_t, prefix))
    down_w = exchange(lambda j: chunk(w_down_t, j))

    own_docs = doc_ids.astype(F32)
    prev_last = jnp.where(place > 0, last[place - 1], -1.0)
    reach_rows = ((own_docs == my_first) & (prev_last == my_first)).astype(F32)[:, None]
    attn = pl.pallas_call(
        functools.partial(out_kernel, heads),
        out_shape=jax.ShapeDtypeStruct((rows, width), BF),
        in_specs=[VMEM] * 7,
        out_specs=VMEM,
        scratch_shapes=[pltpu.VMEM((rows, heads * dv), BF)],
        cost_estimate=pl.CostEstimate(flops=10**9, bytes_accessed=6 * 10**6, transcendentals=0),
    )(o_local, q_dec, prefix, reach_rows, out_gate, head_gain, w_out)

    tp = lax.axis_size("tp")
    share = rows // tp
    core = lax.axis_index("tp")
    attn_sum = tp_scatter(attn.reshape(tp, share, width))
    own_rows = lax.dynamic_slice_in_dim(residual, core * share, share, 0)
    stream = (own_rows.astype(F32) + attn_sum).astype(BF)
    stream_f = stream.astype(F32)
    normed = (stream_f * lax.rsqrt(jnp.mean(stream_f * stream_f, axis=-1, keepdims=True) + EPS) * ffn_gain).astype(BF)
    normed = normed.reshape(share, b, m, depth).transpose(0, 2, 1, 3).reshape(share, width)
    blocks = ordered(normed, [rotate(normed, count, m, b, k) for k in range(1, b)], z, b)
    full = tp_gather(blocks).transpose(1, 0, 2, 3).reshape(b * rows, width)
    ups = jnp.dot(full, up_w, preferred_element_type=F32).astype(BF).reshape(b, rows, 2 * fc)

    tails = rotate(ups[:, -2:], count, 1, m, 1)
    lead = jnp.where(r == 0, jnp.roll(tails, 1, axis=0), tails)
    ext = jnp.concatenate([lead, ups], axis=1).astype(F32)
    at = jnp.arange(b) * m + r
    block_docs = docs[at]
    prev = jnp.where((at > 0)[:, None], docs[(at - 1) % count][:, -2:], -1.0)
    doc_ext = jnp.concatenate([prev, block_docs], axis=1)
    one = (doc_ext[:, 1:-1] == block_docs).astype(F32)[:, :, None]
    two = (doc_ext[:, :-2] == block_docs).astype(F32)[:, :, None]
    taps = lax.dynamic_slice_in_dim(conv_taps, z * fc, fc, 2).reshape(3, 2 * fc)
    bias = lax.dynamic_slice_in_dim(conv_bias, z * fc, fc, 1).reshape(2 * fc)
    mix = bias + taps[2] * ext[:, 2:] + taps[1] * ext[:, 1:-1] * one + taps[0] * ext[:, :-2] * two
    gate_mix, value_mix = mix[..., :fc], mix[..., fc:]
    hidden = (jax.nn.silu(gate_mix) * value_mix).astype(BF).reshape(b * rows, fc)
    partial = nt(hidden, down_w).astype(BF)

    partial = partial.reshape(b, tp, share, width).transpose(1, 0, 2, 3)
    pair = tp_scatter(partial).astype(BF)
    total = lax.dynamic_index_in_dim(pair, z, 0, False).astype(F32)
    for k in range(1, b):
        total += rotate(lax.dynamic_index_in_dim(pair, (z + k) % b, 0, False), count, m, b, k).astype(F32)
    total = total.reshape(share, m, b, depth).transpose(0, 2, 1, 3).reshape(share, width)
    finished = (stream_f + total).astype(BF)
    return tp_gather(finished).reshape(rows, width)


def solution(mesh):
    placed = (
        P("sp", None), P("sp", "tp"), P("sp", "tp"), P("sp", "tp"), P("sp", "tp"), P("sp", "tp"),
        P("sp"), P("tp", None), P("tp", None), P(), P("sp", "tp"), P("sp", "tp"), P("sp", "tp"),
        P(None, None, "tp"), P(None, "tp"),
    )
    return jax.shard_map(per_device, mesh=mesh, in_specs=placed, out_specs=P("sp", None), check_vma=False)
```

```python
import functools

import jax
import jax.numpy as jnp
from jax import lax
from jax.experimental import pallas as pl
from jax.experimental.pallas import tpu as pltpu
from jax.sharding import PartitionSpec as P

EPS = 1e-06
VMEM = pl.BlockSpec(memory_space=pltpu.VMEM)
HIGH = lax.Precision.HIGHEST
BF = jnp.bfloat16
F32 = jnp.float32


def plane_count(positions, hidden):
    return max(b for b in (1, 2, 4) if positions % b == 0 and (hidden // b) % 128 == 0)


def nt(a, b):
    return lax.dot_general(a, b, (((1,), (1,)), ((), ())), preferred_element_type=F32)


def tn(a, b):
    return lax.dot_general(a, b, (((0,), (0,)), ((), ())), preferred_element_type=F32)


def local_kernel(heads, q_ref, k_ref, v_ref, g_ref, dcol_ref, drow_ref, o_ref, s_ref, qd_ref, cum_ref):
    rows = q_ref.shape[0]
    dk = q_ref.shape[1] // heads
    dv = v_ref.shape[1] // heads
    half = rows // 2
    t = lax.broadcasted_iota(jnp.int32, (rows, rows), 0)
    s = lax.broadcasted_iota(jnp.int32, (rows, rows), 1)
    tril = (t >= s).astype(F32)
    cum_ref[...] = jnp.dot(tril, g_ref[...], precision=HIGH, preferred_element_type=F32)
    dcol = dcol_ref[...]
    allowed = (t >= s) & (dcol == drow_ref[...])
    tail = (dcol == dcol_ref[rows - 1:rows, :]).astype(F32)
    scale = dk ** -0.5
    for h in range(heads):
        kc = pl.ds(h * dk, dk)
        vc = pl.ds(h * dv, dv)
        cum = cum_ref[:, kc]
        q = q_ref[:, kc].astype(F32) * scale
        k = k_ref[:, kc].astype(F32)
        v = v_ref[:, vc]
        total = cum[rows - 1:rows, :]
        qd_ref[:, kc] = (q * jnp.exp(cum)).astype(BF)
        s_ref[kc, :] = tn((k * jnp.exp(total - cum) * tail).astype(BF), v).astype(BF)
        edge = cum[half - 1:half, :]
        for part in range(2):
            rs = slice(part * half, (part + 1) * half)
            mid = cum[part * half + half // 2 - 1:part * half + half // 2, :]
            qs = (q[rs] * jnp.exp(cum[rs] - mid)).astype(BF)
            ks = (k[rs] * jnp.exp(mid - cum[rs])).astype(BF)
            a = jnp.where(allowed[rs, rs], nt(qs, ks), 0.0).astype(BF)
            o = jnp.dot(a, v[rs], preferred_element_type=F32)
            if part == 1:
                qx = (q[rs] * jnp.exp(cum[rs] - edge)).astype(BF)
                kx = (k[:half] * jnp.exp(edge - cum[:half])).astype(BF)
                x = jnp.where(allowed[rs, :half], nt(qx, kx), 0.0).astype(BF)
                o = o + jnp.dot(x, v[:half], preferred_element_type=F32)
            o_ref[rs, vc] = o


def out_kernel(heads, o_ref, qd_ref, p_ref, reach_ref, gate_ref, gain_ref, w_ref, out_ref, mixed):
    dk = qd_ref.shape[1] // heads
    dv = o_ref.shape[1] // heads
    for h in range(heads):
        kc = pl.ds(h * dk, dk)
        vc = pl.ds(h * dv, dv)
        carried = jnp.dot(qd_ref[:, kc], p_ref[kc, :], preferred_element_type=F32)
        head = o_ref[:, vc] + carried * reach_ref[...]
        head = head * lax.rsqrt(jnp.mean(head * head, axis=-1, keepdims=True) + EPS) * gain_ref[h:h + 1, :]
        gate = gate_ref[:, vc].astype(F32)
        mixed[:, vc] = (head * gate / (1.0 + jnp.exp(-gate))).astype(BF)
    out_ref[...] = jnp.dot(mixed[...], w_ref[...], preferred_element_type=F32).astype(BF)


def rotate(value, count, stride_in, size, steps):
    perm = []
    for i in range(count):
        d = (i // stride_in) % size
        perm.append((i, i + (((d + steps) % size) - d) * stride_in))
    return lax.ppermute(value, "sp", perm)


def swap(value):
    n = lax.axis_size("tp")
    return [lax.ppermute(value, "tp", [(i, (i + k) % n) for i in range(n)]) for k in range(1, n)]


def tp_gather(value):
    n = lax.axis_size("tp")
    if n != 2:
        return lax.all_gather(value, "tp", axis=0)
    (other,) = swap(value)
    first = lax.axis_index("tp") == 0
    return jnp.stack([jnp.where(first, value, other), jnp.where(first, other, value)])


def tp_scatter(value):
    n = lax.axis_size("tp")
    if n != 2:
        return lax.psum_scatter(value, "tp", scatter_dimension=0, tiled=False).astype(F32)
    c = lax.axis_index("tp")
    give = lax.dynamic_index_in_dim(value, 1 - c, 0, False)
    keep = lax.dynamic_index_in_dim(value, c, 0, False)
    return keep.astype(F32) + swap(give)[0].astype(F32)


def ordered(own, received, place, size):
    buf = jnp.zeros((size,) + own.shape, own.dtype)
    buf = lax.dynamic_update_index_in_dim(buf, own, place, 0)
    for k, item in enumerate(received, 1):
        buf = lax.dynamic_update_index_in_dim(buf, item, (place - k) % size, 0)
    return buf


def plane_gather(block, count, m, r, groups):
    b, depth, columns = block.shape
    if m != 4 or b % 2:
        got = lax.all_gather(block, "sp", axis=0, axis_index_groups=groups)
        return got.transpose(1, 0, 2, 3).reshape(b * m * depth, columns)
    half = b // 2
    near = rotate(block, count, 1, 2, 1)
    far = rotate(block, count, 2, 2, 1)
    diag_top = rotate(near[:half], count, 2, 2, 1)
    diag_low = rotate(far[half:], count, 1, 2, 1)
    x, y = r % 2, r // 2
    buf = jnp.zeros((b, m, depth, columns), block.dtype)

    def put(buf, item, first, i, j):
        return lax.dynamic_update_slice(buf, item[:, None], (first, 2 * j + i, 0, 0))

    buf = put(buf, block, 0, x, y)
    buf = put(buf, near, 0, 1 - x, y)
    buf = put(buf, far, 0, x, 1 - y)
    buf = put(buf, diag_top, 0, 1 - x, 1 - y)
    buf = put(buf, diag_low, half, 1 - x, 1 - y)
    return buf.reshape(b * m * depth, columns)


def per_device(residual, query_proj, key_proj, value_proj, out_gate, log_decay, doc_ids, head_gain,
               w_out, ffn_gain, w_gate, w_value, w_down_t, conv_taps, conv_bias):
    count = lax.axis_size("sp")
    rows = doc_ids.shape[0]
    heads = head_gain.shape[0]
    dk = query_proj.shape[1] // heads
    dv = value_proj.shape[1] // heads
    depth, hidden_here = w_gate.shape
    width = residual.shape[1]
    b = plane_count(count, hidden_here)
    m = count // b
    fc = hidden_here // b
    place = lax.axis_index("sp")
    z, r = place // m, place % m
    groups = [[g * m + i for i in range(m)] for g in range(b)]

    note = jnp.concatenate([jnp.sum(log_decay, axis=0), doc_ids.astype(F32)])
    if b == 1:
        notes = lax.all_gather(note, "sp", axis=0)
    else:
        note = note[None]
        plane = ordered(note, [rotate(note, count, 1, m, k) for k in range(1, m)], r, m)
        notes = ordered(plane, [rotate(plane, count, m, b, k) for k in range(1, b)], z, b)
        notes = notes.reshape(count, -1)
    w_gate, w_value, notes = lax.optimization_barrier((w_gate, w_value, notes))

    def chunk(w, j):
        return lax.dynamic_slice_in_dim(w, j * fc, fc, 1)

    def exchange(pick):
        received = [rotate(pick((z + k) % b), count, m, b, k) for k in range(1, b)]
        block = ordered(pick(z), received, z, b)
        return plane_gather(block, count, m, r, groups)

    up_w = exchange(lambda j: jnp.concatenate([chunk(w_gate, j), chunk(w_value, j)], axis=1))

    totals, docs = notes[:, :heads * dk], notes[:, heads * dk:]
    first, last = docs[:, 0], docs[:, -1]
    steps = jnp.arange(count)

    o_local, state, q_dec = pl.pallas_call(
        functools.partial(local_kernel, heads),
        out_shape=(
            jax.ShapeDtypeStruct((rows, heads * dv), F32),
            jax.ShapeDtypeStruct((heads * dk, dv), BF),
            jax.ShapeDtypeStruct((rows, heads * dk), BF),
        ),
        in_specs=[VMEM] * 6,
        out_specs=(VMEM,) * 3,
        scratch_shapes=[pltpu.VMEM((rows, heads * dk), F32)],
        cost_estimate=pl.CostEstimate(flops=10**9, bytes_accessed=3 * 10**6, transcendentals=0),
    )(query_proj, key_proj, value_proj, log_decay, doc_ids[:, None], doc_ids[None, :])

    if b > 1:
        state, _ = lax.optimization_barrier((state, plane))

    def weight(source, until):
        inside = (steps > source) & (steps < until)
        return jnp.exp(jnp.sum(jnp.where(inside[:, None], totals, 0.0), axis=0))

    my_first = first[place]
    if b == 1:
        all_states = lax.all_gather(state, "sp", axis=0)

        def add(i, acc):
            live = (i < place) & (last[i] == my_first)
            scale = jnp.where(live, weight(i, place), 0.0)
            return acc + scale[:, None] * all_states[i].astype(F32)

        prefix = lax.fori_loop(0, count, add, jnp.zeros(state.shape, F32))
    else:
        near = [state] + [rotate(state, count, 1, m, k) for k in range(1, m)]
        end = (z + 1) * m
        start = z * m
        rows_of = []
        for k in range(1, m):
            source = start + (r - k) % m
            rows_of.append((source, place, (source < place) & (last[source] == my_first)))
        for k in range(m):
            source = start + (r - k) % m
            rows_of.append((source, end, last[source] == last[end - 1]))
        for k in range(1, b):
            source = jnp.maximum(z - k + 1, 0) * m - 1
            rows_of.append((source, start, (z >= k) & (last[source] == first[start])))
        rows_of.append((start - 1, place, first[start] == my_first))
        sources, untils, lives = (jnp.stack(col)[:, None] for col in zip(*rows_of))
        inside = ((steps > sources) & (steps < untils)).astype(F32)
        gaps = lax.dot_general(totals, inside, (((0,), (1,)), ((), ())), precision=HIGH,
                               preferred_element_type=F32)
        scales = jnp.where(lives[:, 0], jnp.exp(jnp.minimum(gaps, 0.0)), 0.0)
        pick_scale = lambda i: scales[:, i:i + 1]
        prefix = sum(pick_scale(k - 1) * near[k].astype(F32) for k in range(1, m))
        plane_end = sum(pick_scale(m - 1 + k) * near[k].astype(F32) for k in range(m)).astype(BF)
        whole = sum(
            pick_scale(2 * m - 2 + k)
            * lax.ppermute(plane_end, "sp", [(i, i + k * m) for i in range(count - k * m)]).astype(F32)
            for k in range(1, b)
        )
        prefix += pick_scale(2 * m - 2 + b) * whole

    prefix = prefix.astype(BF)
    w_down_t, prefix = lax.optimization_barrier((w_down_t, prefix))
    down_w = exchange(lambda j: chunk(w_down_t, j))

    own_docs = doc_ids.astype(F32)
    prev_last = jnp.where(place > 0, last[place - 1], -1.0)
    reach_rows = ((own_docs == my_first) & (prev_last == my_first)).astype(F32)[:, None]
    attn = pl.pallas_call(
        functools.partial(out_kernel, heads),
        out_shape=jax.ShapeDtypeStruct((rows, width), BF),
        in_specs=[VMEM] * 7,
        out_specs=VMEM,
        scratch_shapes=[pltpu.VMEM((rows, heads * dv), BF)],
        cost_estimate=pl.CostEstimate(flops=10**9, bytes_accessed=6 * 10**6, transcendentals=0),
    )(o_local, q_dec, prefix, reach_rows, out_gate, head_gain, w_out)

    tp = lax.axis_size("tp")
    share = rows // tp
    core = lax.axis_index("tp")
    attn_sum = tp_scatter(attn.reshape(tp, share, width))
    own_rows = lax.dynamic_slice_in_dim(residual, core * share, share, 0)
    stream = (own_rows.astype(F32) + attn_sum).astype(BF)
    stream_f = stream.astype(F32)
    normed = (stream_f * lax.rsqrt(jnp.mean(stream_f * stream_f, axis=-1, keepdims=True) + EPS) * ffn_gain).astype(BF)
    blocks = ordered(normed, [rotate(normed, count, m, b, k) for k in range(1, b)], z, b)
    full = tp_gather(blocks).transpose(1, 0, 2, 3).reshape(b * rows, width)
    ups = jnp.dot(full, up_w, preferred_element_type=F32).astype(BF).reshape(b, rows, 2 * fc)

    tails = rotate(ups[:, -2:], count, 1, m, 1)
    lead = jnp.where(r == 0, jnp.roll(tails, 1, axis=0), tails)
    ext = jnp.concatenate([lead, ups], axis=1).astype(F32)
    at = jnp.arange(b) * m + r
    block_docs = docs[at]
    prev = jnp.where((at > 0)[:, None], docs[(at - 1) % count][:, -2:], -1.0)
    doc_ext = jnp.concatenate([prev, block_docs], axis=1)
    one = (doc_ext[:, 1:-1] == block_docs).astype(F32)[:, :, None]
    two = (doc_ext[:, :-2] == block_docs).astype(F32)[:, :, None]
    taps = lax.dynamic_slice_in_dim(conv_taps, z * fc, fc, 2).reshape(3, 2 * fc)
    bias = lax.dynamic_slice_in_dim(conv_bias, z * fc, fc, 1).reshape(2 * fc)
    mix = bias + taps[2] * ext[:, 2:] + taps[1] * ext[:, 1:-1] * one + taps[0] * ext[:, :-2] * two
    gate_mix, value_mix = mix[..., :fc], mix[..., fc:]
    hidden = (jax.nn.silu(gate_mix) * value_mix).astype(BF).reshape(b * rows, fc)
    partial = nt(hidden, down_w).astype(BF)

    partial = partial.reshape(b, tp, share, width).transpose(1, 0, 2, 3)
    pair = tp_scatter(partial).astype(BF)
    total = lax.dynamic_index_in_dim(pair, z, 0, False).astype(F32)
    for k in range(1, b):
        total += rotate(lax.dynamic_index_in_dim(pair, (z + k) % b, 0, False), count, m, b, k).astype(F32)
    finished = (stream_f + total).astype(BF)
    return tp_gather(finished).reshape(rows, width)


def solution(mesh):
    placed = (
        P("sp", None), P("sp", "tp"), P("sp", "tp"), P("sp", "tp"), P("sp", "tp"), P("sp", "tp"),
        P("sp"), P("tp", None), P("tp", None), P(), P("sp", "tp"), P("sp", "tp"), P("sp", "tp"),
        P(None, None, "tp"), P(None, "tp"),
    )
    return jax.shard_map(per_device, mesh=mesh, in_specs=placed, out_specs=P("sp", None), check_vma=False)
```
